32 devices in a mesh: ep: 16 (over z, y, core), tp: 2 (over x).
Axes of the slice: x: 2, y: 2, z: 4, core: 2. Of those that a mesh axis runs over, the one named last changes fastest.
Arguments:
- tokens: bfloat16 [128, 2048], P('ep'), may hold values from -48 to 48
- past_lengths: int32 [128], P('ep'), may hold values from 1024 to 16383
- state: float32 [128, 16, 128, 256], P('ep', 'tp'), may hold values from -0.625 to 0.625
- norm1_gain: float32 [2048], replicated, may hold values from 0.1 to 1.9
- query_weight: bfloat16 [2048, 2048], P(None, 'tp'), may hold values from -0.125 to 0.125
- key_weight: bfloat16 [2048, 2048], P(None, 'tp'), may hold values from -0.125 to 0.125
- value_weight: bfloat16 [2048, 4096], P(None, 'tp'), may hold values from -0.125 to 0.125
- out_weight: bfloat16 [4096, 2048], P('tp'), may hold values from -0.09375 to 0.09375
- norm2_gain: float32 [2048], replicated, may hold values from 0.1 to 1.9
- branch_gate: float32 [2048], replicated, may hold values from -0.125 to 0.125
- route_ids: int32 [128, 2], P('ep'), may hold values from 0 to 3, all different within a row; in each aligned block of 8 rows (0 to 7, 8 to 15, ...) at most 8 rows name the same one
- route_weights: float32 [128, 2], P('ep'), may hold values from 0.2 to 1
- expert_gate: bfloat16 [16, 2048, 1792], P('ep', None, 'tp'), may hold values from -0.125 to 0.125
- expert_up: bfloat16 [16, 2048, 1792], P('ep', None, 'tp'), may hold values from -0.125 to 0.125
- expert_down: bfloat16 [16, 1792, 2048], P('ep', 'tp'), may hold values from -0.0625 to 0.0625
- dense_gate: bfloat16 [2048, 5632], P('tp', 'ep'), may hold values from -0.125 to 0.125
- dense_up: bfloat16 [2048, 5632], P('tp', 'ep'), may hold values from -0.125 to 0.125
- dense_down: bfloat16 [5632, 2048], P('ep', 'tp'), may hold values from -0.15625 to 0.15625
Outputs:
- layer_out: bfloat16 [128, 2048], P('ep', 'tp')
- new_state: float32 [128, 16, 128, 256], P('ep', 'tp')
The draws below stay inside these ranges and needn't reach their ends.
Inputs may be any that keep to these rules, and one draw needn't show every extreme that they name: `route_ids`: in each aligned block of 8 rows no expert is named by more than 8 rows, and some block names one expert exactly 8 times.
All inputs are finite; a program needn't handle non-finite values.
Results may differ from the reference program's by a relative error of at most 0.006.
Values may be sent and summed in bfloat16 or wider, within the bound.
A program may use at most 128 MiB of HBM per device.

```python
import math
import jax
import jax.numpy as jnp
import numpy as np
from jax import lax

G = 8
TOKENS = 128
D = 2048
H = 16
DK = 128
DV = 256
FF = 5632
EXP_FF = 7168
TOPK = 2
EXPERTS = 4
CAP = 8


def draw_tokens(key, part):
    first_key, second_key = jax.random.split(jax.random.fold_in(key, 11), 2)
    columns = jnp.arange(D, dtype=jnp.float32) / D
    base = jax.random.truncated_normal(first_key, -4.0, 4.0, (TOKENS, D), jnp.float32)
    col_scale = jnp.exp(jnp.log(3.0) * columns)
    row_scale = jnp.exp(jax.random.uniform(second_key, (TOKENS, 1), jnp.float32, jnp.log(0.5), jnp.log(3.0)))
    return (base * col_scale[None, :] * row_scale).astype(jnp.bfloat16)


def touch_ends(result, rng, low, top_value):
    longest = result.shape.index(max(result.shape))
    spots = []
    for shift in (0, 1):
        where = [jax.random.randint(jax.random.fold_in(rng, axis), (), 0, length) for axis, length in enumerate(result.shape)]
        where[longest] = (where[longest] + shift) % result.shape[longest]
        spots.append(tuple(where))
    return result.at[spots[0]].set(low).at[spots[1]].set(top_value)


def shard_levels(rng, shape, cuts, smallest, high):
    def one(position, parts):
        steps = jax.random.uniform(jax.random.fold_in(jax.random.fold_in(rng, 6), position), (parts,), jnp.float32, smallest / len(cuts), high / len(cuts))
        return jnp.repeat(jnp.exp(steps), shape[position] // parts).reshape((-1,) + (1,) * (len(shape) - position - 1))

    factor_of = one(*cuts[0])
    for cut in cuts[1:]:
        factor_of = factor_of * one(*cut)
    return factor_of


def assign_block(stream_key, own, number, rows, amount, top, limit, lean):
    order = jax.random.permutation(stream_key, amount)
    packed, ordinary = shares(amount, rows * top, limit, lean, True), shares(amount, rows * top, limit, lean, False)
    places = jnp.arange(amount)

    def named(lengths, turn):
        used = int((lengths > 0).sum())
        fixed = max(1, used // 4)
        moved = fixed + (places - fixed + turn * (used - fixed)) % max(1, amount - fixed)
        return jnp.zeros((amount,), jnp.int32).at[order[jnp.where(places < fixed, places, moved)]].set(jnp.asarray(lengths, jnp.int32))

    lengths = jnp.where(number % 4 == 0, named(packed, number // 4), named(ordinary, number - number // 4 - 1))
    mixed = jax.random.permutation(jax.random.fold_in(own, 3), amount)
    source_of, sink = mixed[0:amount // 2 * 2:2], mixed[1:amount // 2 * 2:2]
    slack = jnp.minimum(lengths[source_of] - 1, limit - lengths[sink]) // 2
    slack = jnp.where((source_of == order[0]) | (sink == order[0]) | (lengths[sink] == 0), 0, jnp.maximum(slack, 0))
    moved = jax.random.randint(jax.random.fold_in(own, 4), (amount // 2,), 0, 1 << 20) % (slack + 1)
    lengths = lengths.at[source_of].add(-moved).at[sink].add(moved)
    members = jnp.searchsorted(jnp.cumsum(lengths), jnp.arange(rows * top), side="right").astype(jnp.int32)
    table = members.reshape(top, rows).T
    table = table[jax.random.permutation(jax.random.fold_in(own, 1), rows)]
    turn = jax.random.randint(jax.random.fold_in(own, 2), (rows, 1), 0, top)
    return jnp.take_along_axis(table, (jnp.arange(top)[None, :] + turn) % top, axis=1)


def shares(count, total, bound, lean, full):
    portions = [(1 << 20) // math.isqrt(rank ** lean) + 1 for rank in range(1, count + 1)]
    largest = bound if full else min(bound, max(-(-total // count), total * portions[0] // sum(portions)))
    least = 1 if total - largest >= count - 1 else 0
    given, spare = [largest] + [least] * (count - 1), total - largest - least * (count - 1)
    while spare > 0:
        free = [i for i in range(1, count) if given[i] < largest] or [i for i in range(1, count) if given[i] < bound]
        pool, left = sum([portions[i] for i in free]), spare
        for i in free:
            extra = min(bound - given[i], max(1, left * portions[i] // pool), spare)
            given[i] = given[i] + extra
            spare = spare - extra
    return np.array(given)


def normal_values(stream_key, shape, deviation, most, cuts=(), kind=jnp.bfloat16):
    drawn = jax.random.normal(stream_key, shape, jnp.float32) * deviation
    if len(cuts) > 0:
        drawn = shard_levels(stream_key, shape, cuts, -0.22, 0.18) * drawn
    return jnp.clip(drawn, min=-most, max=most).astype(kind)


def setup_inputs(seed: int = 0) -> dict:
    streams_of = jax.random.split(jax.random.key(seed), 19)
    tokens = draw_tokens(jax.random.fold_in(streams_of[18], 71), 0)
    past_lengths = touch_ends(jax.random.randint(streams_of[1], (TOKENS,), 1024, 16384), jax.random.fold_in(streams_of[1], 1), 1024, 16383).astype(jnp.int32)
    state = normal_values(streams_of[2], (TOKENS, H, DK, DV), 0.1, 0.625, ((0, 16), (1, 2)), jnp.float32)
    norm1_gain = jnp.clip(1.0 + 0.18 * jax.random.normal(streams_of[3], (D,), jnp.float32), 0.1, 1.9)
    query_weight = normal_values(streams_of[4], (D, H * DK), D ** -0.5, 0.125, ((1, 2),))
    key_weight = normal_values(streams_of[5], (D, H * DK), D ** -0.5, 0.125, ((1, 2),))
    value_weight = normal_values(streams_of[6], (D, H * DV), D ** -0.5, 0.125, ((1, 2),))
    out_weight = normal_values(streams_of[7], (H * DV, D), (H * DV) ** -0.5, 0.09375, ((0, 2),))
    norm2_gain = jnp.clip(1.0 + 0.18 * jax.random.normal(streams_of[8], (D,), jnp.float32), 0.1, 1.9)
    branch_gate = normal_values(streams_of[9], (D,), D ** -0.5, 0.125, (), jnp.float32)
    route_ids_keys = jax.random.split(jax.random.fold_in(streams_of[10], 1), TOKENS // G)
    route_ids_turns = jax.random.permutation(jax.random.fold_in(streams_of[10], 3), TOKENS // G)
    route_ids = jax.vmap(lambda own, number: assign_block(jax.random.fold_in(streams_of[10], 2), own, number, G, EXPERTS, TOPK, CAP, 1))(route_ids_keys, route_ids_turns).reshape((TOKENS, TOPK))
    route_weights = jnp.clip(0.2 + 0.8 * jax.random.uniform(streams_of[11], (TOKENS, TOPK), jnp.float32) ** shard_levels(streams_of[11], (TOKENS, TOPK), ((0, 16),), -0.2, 0.2), 0.2, 1.0)
    expert_gate = normal_values(streams_of[12], (4 * EXPERTS, D, EXP_FF // 4), D ** -0.5, 0.125, ((0, 16), (2, 2)))
    expert_up = normal_values(streams_of[13], (4 * EXPERTS, D, EXP_FF // 4), D ** -0.5, 0.125, ((0, 16), (2, 2)))
    expert_down = normal_values(streams_of[14], (4 * EXPERTS, EXP_FF // 4, D), EXP_FF ** -0.5, 0.0625, ((0, 16), (1, 2)))
    dense_gate = normal_values(streams_of[15], (D, FF), D ** -0.5, 0.125, ((0, 2), (1, 16)))
    dense_up = normal_values(streams_of[16], (D, FF), D ** -0.5, 0.125, ((0, 2), (1, 16)))
    dense_down = normal_values(streams_of[17], (FF, D), (FF // 4) ** -0.5, 0.15625, ((0, 16), (1, 2)))
    return {"tokens": tokens, "past_lengths": past_lengths, "state": state, "norm1_gain": norm1_gain, "query_weight": query_weight, "key_weight": key_weight, "value_weight": value_weight, "out_weight": out_weight, "norm2_gain": norm2_gain, "branch_gate": branch_gate, "route_ids": route_ids, "route_weights": route_weights, "expert_gate": expert_gate, "expert_up": expert_up, "expert_down": expert_down, "dense_gate": dense_gate, "dense_up": dense_up, "dense_down": dense_down}


RMS_EPSILON = 1e-06
GROUP_EPSILON = 1e-05
PRECISE = lax.Precision.HIGHEST

def head_decay(head_index, head_total):
    return jnp.exp(jnp.log1p(-jnp.exp2(-5.0 - 7.0 * head_index.astype(jnp.float32) / (head_total - 1))))

def rotate_heads(features, positions):
    half_size = features.shape[-1] // 2
    inverse = 10000.0 ** (-jnp.arange(half_size, dtype=jnp.float32) / half_size)
    angles = positions.astype(jnp.float32)[:, None] * inverse[None, :]
    cosine = jnp.cos(angles)[:, None, :]
    sine_part = jnp.sin(angles)[:, None, :]
    first_half = features[..., :half_size]
    second_half = features[..., half_size:]
    return jnp.concatenate([first_half * cosine - second_half * sine_part, first_half * sine_part + second_half * cosine], axis=-1)

def retention_step(normed_in, positions, state, query_weight, key_weight, value_weight, head_index, head_total):
    row_count, head_count, key_size, value_size = state.shape
    query = jnp.dot(normed_in, query_weight, preferred_element_type=jnp.float32).reshape(row_count, head_count, key_size)
    keys = jnp.dot(normed_in, key_weight, preferred_element_type=jnp.float32).reshape(row_count, head_count, key_size)
    values = jnp.dot(normed_in, value_weight, preferred_element_type=jnp.float32).reshape(row_count, head_count, value_size)
    query = rotate_heads(query, positions)
    keys = rotate_heads(keys, positions) * key_size ** (-0.5)
    decay = head_decay(head_index, head_total)
    new_state = state * decay[None, :, None, None] + keys[:, :, :, None] * values[:, :, None, :]
    retained = jnp.einsum('shk,shkv->shv', query, new_state, precision=PRECISE)
    centered = retained - lax.optimization_barrier(jnp.mean(retained, axis=-1, keepdims=True))
    normed = centered * lax.rsqrt(lax.optimization_barrier(jnp.mean(centered * centered, axis=-1, keepdims=True)) + GROUP_EPSILON)
    return (normed.astype(jnp.bfloat16).reshape(row_count, head_count * value_size), new_state)

def reference(tokens, past_lengths, state, norm1_gain, query_weight, key_weight, value_weight, out_weight, norm2_gain, branch_gate, route_ids, route_weights, expert_gate, expert_up, expert_down, dense_gate, dense_up, dense_down):
    inputs = tokens.astype(jnp.float32)
    normed_in = (inputs * lax.rsqrt(lax.optimization_barrier(jnp.mean(inputs * inputs, axis=-1, keepdims=True)) + RMS_EPSILON) * norm1_gain).astype(jnp.bfloat16)
    head_total = state.shape[1]
    normed, new_state = retention_step(normed_in, past_lengths, state, query_weight, key_weight, value_weight, jnp.arange(head_total), head_total)
    mixed = inputs + jnp.dot(normed, out_weight, preferred_element_type=jnp.float32)
    scale = lax.rsqrt(lax.optimization_barrier(jnp.mean(mixed * mixed, axis=-1, keepdims=True)) + RMS_EPSILON)
    scaled = mixed * scale * norm2_gain
    branch_weight = jax.nn.sigmoid(lax.optimization_barrier(jnp.sum(scaled * branch_gate, axis=-1, keepdims=True)))
    normed_out = scaled.astype(jnp.bfloat16)
    model_width = tokens.shape[1]
    group_count = tokens.shape[0] // G
    route_flat = route_ids.reshape(group_count, G * TOPK)
    onehot = (route_flat[:, :, None] == jnp.arange(EXPERTS, dtype=jnp.int32)[None, None, :]).astype(jnp.int32)
    earlier = jnp.cumsum(onehot, axis=1) - onehot
    slot_index = lax.optimization_barrier(jnp.sum(earlier * onehot, axis=2))
    target = route_flat * CAP + slot_index
    placed = (target[:, :, None] == jnp.arange(EXPERTS * CAP, dtype=jnp.int32)[None, None, :]).astype(jnp.float32)
    placed = placed.reshape(group_count, G, TOPK, EXPERTS * CAP)
    selector = lax.optimization_barrier(jnp.sum(placed, axis=2))
    combiner = lax.optimization_barrier(jnp.sum(placed * route_weights.reshape(group_count, G, TOPK, 1), axis=2))
    grouped = normed_out.reshape(group_count, G, model_width).astype(jnp.float32)
    buffers = jnp.einsum('gtp,gtd->gpd', selector, grouped, precision=PRECISE).astype(jnp.bfloat16)
    expert_rows = buffers.reshape(group_count, EXPERTS, CAP, model_width).transpose(1, 0, 2, 3).reshape(EXPERTS, group_count * CAP, model_width)
    quarter = expert_gate.shape[2]
    gate_full = expert_gate.reshape(EXPERTS, 4, model_width, quarter).transpose(0, 2, 1, 3).reshape(EXPERTS, model_width, 4 * quarter)
    up_full = expert_up.reshape(EXPERTS, 4, model_width, quarter).transpose(0, 2, 1, 3).reshape(EXPERTS, model_width, 4 * quarter)
    down_full = expert_down.reshape(EXPERTS, 4 * quarter, model_width)

    def one_expert(pieces):
        rows, gate_w, up_w, down_w = pieces
        gate_value = jnp.dot(rows, gate_w, preferred_element_type=jnp.float32)
        up_value = jnp.dot(rows, up_w, preferred_element_type=jnp.float32)
        hidden = (jax.nn.silu(gate_value) * up_value).astype(jnp.bfloat16)
        return jnp.dot(hidden, down_w, preferred_element_type=jnp.float32)
    expert_out = lax.map(one_expert, (expert_rows, gate_full, up_full, down_full))
    per_group = expert_out.reshape(EXPERTS, group_count, CAP, model_width).transpose(1, 0, 2, 3).reshape(group_count, EXPERTS * CAP, model_width)
    routed = jnp.einsum('gtp,gpd->gtd', combiner, per_group, precision=PRECISE).reshape(-1, model_width)
    dense_gate_value = jnp.dot(normed_out, dense_gate, preferred_element_type=jnp.float32)
    dense_up_value = jnp.dot(normed_out, dense_up, preferred_element_type=jnp.float32)
    dense_hidden = (jax.nn.silu(dense_gate_value) * dense_up_value).astype(jnp.bfloat16)
    dense_result = jnp.dot(dense_hidden, dense_down, preferred_element_type=jnp.float32)
    layer_out = (mixed + routed + branch_weight * dense_result).astype(jnp.bfloat16)
    return (layer_out, new_state)
```

```python
import functools

import jax
import jax.numpy as jnp
from jax import lax
from jax.experimental import pallas as pl
from jax.experimental.pallas import tpu as pltpu
from jax.sharding import PartitionSpec as P

MESH = pl.DeviceIdType.MESH

RMS_EPSILON = 1e-06
GROUP_EPSILON = 1e-05


def head_decay(head_index, head_total):
    return jnp.exp(
        jnp.log1p(-jnp.exp2(-5.0 - 7.0 * head_index.astype(jnp.float32) / (head_total - 1)))
    )


def rotate_heads(features, positions):
    half_size = features.shape[-1] // 2
    inverse = 10000.0 ** (-jnp.arange(half_size, dtype=jnp.float32) / half_size)
    angles = positions.astype(jnp.float32)[:, None] * inverse[None, :]
    cosine = jnp.cos(angles)[:, None, :]
    sine_part = jnp.sin(angles)[:, None, :]
    first_half = features[..., :half_size]
    second_half = features[..., half_size:]
    return jnp.concatenate(
        [
            first_half * cosine - second_half * sine_part,
            first_half * sine_part + second_half * cosine,
        ],
        axis=-1,
    )


def retention_step(
    normed_in, positions, state, query_weight, key_weight, value_weight, head_index, head_total
):
    row_count, head_count, key_size, value_size = state.shape
    query = jnp.dot(normed_in, query_weight, preferred_element_type=jnp.float32).reshape(
        row_count, head_count, key_size
    )
    keys = jnp.dot(normed_in, key_weight, preferred_element_type=jnp.float32).reshape(
        row_count, head_count, key_size
    )
    values = jnp.dot(normed_in, value_weight, preferred_element_type=jnp.float32).reshape(
        row_count, head_count, value_size
    )
    query = rotate_heads(query, positions)
    keys = rotate_heads(keys, positions) * key_size ** (-0.5)
    decay = head_decay(head_index, head_total)
    new_state = state * decay[None, :, None, None] + keys[:, :, :, None] * values[:, :, None, :]
    retained = jnp.einsum("shk,shkv->shv", query, new_state)
    centered = retained - jnp.mean(retained, axis=-1, keepdims=True)
    normed = centered * lax.rsqrt(
        jnp.mean(centered * centered, axis=-1, keepdims=True) + GROUP_EPSILON
    )
    return (normed.astype(jnp.bfloat16).reshape(row_count, head_count * value_size), new_state)


LANES = 128
HALF = LANES // 2
LAST_DIMS = (((1,), (1,)), ((), ()))


def await_bytes(ref, semaphore):
    pltpu.make_async_copy(ref, ref, semaphore).wait()


QUARTERS = 4
CHUNK = 512


def other_index(index, count, step):
    if count & (count - 1):
        return lax.rem(index + step, count)
    result = 0
    for bit in range(count.bit_length() - 1):
        own = lax.rem(lax.div(index, 1 << bit), 2)
        result = result + lax.rem(own + ((step >> bit) & 1), 2) * (1 << bit)
    return result


def tail_kernel(
    ep_count,
    tp_count,
    heads_ref,
    token_ref,
    gain_ref,
    gate_ref,
    route_ref,
    out_weight,
    expert_gate,
    expert_up,
    expert_down,
    dense_gate,
    dense_up,
    dense_down,
    out_ref,
    out_w,
    pair_w,
    down_w,
    dense_gate_w,
    dense_up_w,
    dense_down_w,
    partial_out,
    partials,
    mixed_ref,
    gathered,
    normed_ref,
    dense_part,
    dense_parts,
    hidden_ref,
    outgoing,
    sibling_in,
    chip_out,
    arrived,
    sems,
    out_sems,
    line_sems,
    plane_sems,
    pair_sems,
):
    ep = lax.axis_index("ep")
    tp = lax.axis_index("tp")
    rows, width = token_ref.shape
    token_count = ep_count * rows
    col_width = width // tp_count
    tiles = pair_w.shape[0]
    experts = ep_count // QUARTERS
    places = 2 * tp_count
    chips = experts * places
    expert = lax.div(ep, QUARTERS)
    upper = lax.rem(lax.div(ep, 2), 2)
    side = lax.rem(ep, 2)
    place = tp * 2 + upper
    chip = expert * places + place
    own_row = expert * 2 + upper
    sibling = (ep + 1 - 2 * side, tp)
    head_width = heads_ref.shape[1]
    head_chunk = min(CHUNK, head_width)
    head_chunks = head_width // head_chunk
    own_cols = pl.ds(pl.multiple_of(tp * col_width, LANES), col_width)

    def device(expert_to, place_to):
        return (
            expert_to * QUARTERS + lax.rem(place_to, 2) * 2 + side,
            lax.div(place_to, 2),
        )

    def send(source, target, send_sem, receive_sem, to):
        pltpu.make_async_remote_copy(
            src_ref=source,
            dst_ref=target,
            send_sem=send_sem,
            recv_sem=receive_sem,
            device_id=to,
            device_id_type=MESH,
        ).start()

    part_order = list(range(1, tp_count)) + [0]
    for k in part_order:
        part = lax.rem(tp + k, tp_count)
        for r in range(head_chunks):
            span = pl.ds(r * head_chunk, head_chunk)
            cols = pl.ds(pl.multiple_of(part * col_width, LANES), col_width)
            pltpu.make_async_copy(
                out_weight.at[span, cols],
                out_w.at[k, span, :],
                out_sems.at[k * head_chunks + r],
            ).start()

    barrier = pltpu.get_barrier_semaphore()

    def greet(k, carry):
        other = lax.rem(chip + k, chips)
        pl.semaphore_signal(
            barrier,
            inc=1,
            device_id=device(lax.div(other, places), lax.rem(other, places)),
            device_id_type=MESH,
        )
        return carry

    lax.fori_loop(1, chips, greet, 0)
    pl.semaphore_signal(barrier, inc=1, device_id=sibling, device_id_type=MESH)

    def copy_tile(j):
        cols = pl.ds(j * LANES, LANES)
        pltpu.make_async_copy(
            expert_gate.at[0, :, cols], pair_w.at[j, :, pl.ds(0, LANES)], sems.at[0]
        ).start()
        pltpu.make_async_copy(
            expert_up.at[0, :, cols], pair_w.at[j, :, pl.ds(LANES, LANES)], sems.at[0]
        ).start()

    pltpu.make_async_copy(dense_gate, dense_gate_w, sems.at[2]).start()
    pltpu.make_async_copy(dense_up, dense_up_w, sems.at[3]).start()
    for j in range(tiles):
        copy_tile(j)
    pltpu.make_async_copy(expert_down.at[0], down_w, sems.at[1]).start()
    pltpu.make_async_copy(dense_down, dense_down_w, sems.at[4]).start()

    for k in part_order:
        part = lax.rem(tp + k, tp_count)
        total = jnp.zeros((rows, col_width), jnp.float32)
        for r in range(head_chunks):
            span = pl.ds(r * head_chunk, head_chunk)
            await_bytes(out_w.at[k, span, :], out_sems.at[k * head_chunks + r])
            total = total + jnp.dot(
                heads_ref[:, span], out_w[k, span, :], preferred_element_type=jnp.float32
            )
        if k:
            partial_out[k - 1] = total
            if k == 1:
                pl.semaphore_wait(barrier, chips)
            send(partial_out.at[k - 1], partials.at[tp], sems.at[5], sems.at[6], (ep, part))
        else:
            partials[tp] = total
    await_bytes(partials.at[pl.ds(0, tp_count - 1)], sems.at[6])

    mixed = token_ref[:, own_cols].astype(jnp.float32) + jnp.sum(partials[...], axis=0)
    mixed_ref[...] = mixed
    raised = mixed * gain_ref[:, own_cols]
    squares = jnp.sum(mixed * mixed, axis=-1, keepdims=True)
    along = jnp.sum(raised * gate_ref[:, own_cols], axis=-1, keepdims=True)
    lane = lax.broadcasted_iota(jnp.int32, (rows, LANES), 1)
    factors = jnp.where(lane == HALF - 1, along, route_ref[...])
    factors = jnp.where(lane == HALF - 2, squares, factors)
    high = factors.astype(jnp.bfloat16).astype(jnp.float32)
    low = pltpu.roll(factors - high, HALF, 1)
    gathered[side, expert, place, :, pl.ds(0, col_width)] = raised.astype(jnp.bfloat16)
    gathered[side, expert, place, :, pl.ds(col_width, LANES)] = jnp.where(
        lane < HALF, high, low
    ).astype(jnp.bfloat16)

    own_block = gathered.at[side, expert, place]
    one_block = gathered.at[0, 0, 0]
    others = [other_index(expert, experts, step) for step in range(1, experts)]
    for other in others:
        send(own_block, own_block, sems.at[7], line_sems.at[expert], device(other, place))

    def to_plane(block_expert):
        block = gathered.at[side, block_expert, place]

        def one(k, carry):
            place_to = lax.rem(place + k, places)
            send(
                block, block, sems.at[8], plane_sems.at[block_expert], device(expert, place_to)
            )
            return carry

        lax.fori_loop(1, places, one, 0)

    to_plane(expert)
    for other in others:
        await_bytes(one_block, line_sems.at[other])
        to_plane(other)
    for block_expert in [expert] + others:
        await_bytes(gathered.at[0, 0, pl.ds(0, places - 1)], plane_sems.at[block_expert])
        send(
            gathered.at[side, block_expert],
            gathered.at[side, block_expert],
            sems.at[9],
            sems.at[10],
            sibling,
        )
    await_bytes(gathered.at[0], sems.at[10])

    lane_place = lax.rem(lax.broadcasted_iota(jnp.int32, (token_count, LANES), 1), HALF)
    summed = jnp.zeros((token_count, LANES), jnp.float32)
    for t in range(tp_count):
        pair = pl.ds(2 * t, 2)
        normed_ref[:, pl.ds(t * col_width, col_width)] = (
            gathered[:, :, pair, :, pl.ds(0, col_width)]
            .astype(jnp.float32)
            .reshape(token_count, col_width)
            .astype(jnp.bfloat16)
        )
        tail_lanes = (
            gathered[:, :, pair, :, pl.ds(col_width, LANES)]
            .astype(jnp.float32)
            .reshape(token_count, LANES)
        )
        summed = summed + tail_lanes

    def lanes_sum(values, where):
        return jnp.sum(jnp.where(lane_place == where, values, 0.0), axis=1, keepdims=True)

    expert_factor = lanes_sum(tail_lanes, expert)
    scale = lax.rsqrt(lanes_sum(summed, HALF - 2) / width + RMS_EPSILON)
    branch_factor = 1.0 / (1.0 + jnp.exp(-scale * lanes_sum(summed, HALF - 1)))

    await_bytes(dense_gate_w, sems.at[2])
    await_bytes(dense_up_w, sems.at[3])
    feature_values = normed_ref[:, own_cols]
    for index, weight in ((0, dense_gate_w), (1, dense_up_w)):
        dense_part[index] = (
            scale
            * lax.dot_general(
                feature_values, weight[...], LAST_DIMS, preferred_element_type=jnp.float32
            )
        ).astype(jnp.bfloat16)
    pltpu.make_async_copy(dense_part, dense_parts.at[tp], sems.at[12]).start()

    def share_dense(k, carry):
        send(
            dense_part,
            dense_parts.at[tp],
            sems.at[11],
            sems.at[12],
            (ep, lax.rem(tp + k, tp_count)),
        )
        return carry

    lax.fori_loop(1, tp_count, share_dense, 0)

    await_bytes(pair_w, sems.at[0])

    def expert_tile(j, carry):
        both = scale * jnp.dot(normed_ref[...], pair_w[j], preferred_element_type=jnp.float32)
        gate_value, up_value = both[:, :LANES], both[:, LANES:]
        hidden_ref[:, pl.ds(pl.multiple_of(j * LANES, LANES), LANES)] = (
            gate_value / (1.0 + jnp.exp(-gate_value)) * up_value
        ).astype(jnp.bfloat16)
        return carry

    lax.fori_loop(0, tiles, expert_tile, 0)
    await_bytes(down_w, sems.at[1])
    step = min(2 * LANES, col_width)

    def expert_cols(part, t):
        cols = pl.ds(pl.multiple_of(part * col_width + t * step, LANES), step)
        return expert_factor * jnp.dot(
            hidden_ref[...], down_w[:, cols], preferred_element_type=jnp.float32
        )

    def put(part, t, value):
        outgoing[part, :, :, :, pl.ds(pl.multiple_of(t * step, LANES), step)] = value.reshape(
            2, 2 * experts, rows, step
        ).astype(jnp.bfloat16)

    def to_sibling(part):
        send(
            outgoing.at[part, 1 - side],
            sibling_in.at[part],
            sems.at[13],
            pair_sems.at[part],
            sibling,
        )

    def send_out(part, first):
        await_bytes(sibling_in.at[part], pair_sems.at[part])
        chip_out[part] = (
            outgoing[part, side].astype(jnp.float32) + sibling_in[part].astype(jnp.float32)
        ).astype(jnp.bfloat16)

        def one(k, carry):
            to = lax.rem(own_row + k, 2 * experts)
            send(
                chip_out.at[part, to],
                arrived.at[chip],
                sems.at[14],
                sems.at[15],
                (to * 2 + side, part),
            )
            return carry

        lax.fori_loop(first, 2 * experts, one, 0)

    def other_part(k, carry):
        part = lax.rem(tp + k, tp_count)

        def tile(t, inner):
            put(part, t, expert_cols(part, t))
            return inner

        lax.fori_loop(0, col_width // step, tile, 0)
        to_sibling(part)
        return carry

    lax.fori_loop(1, tp_count, other_part, 0)

    await_bytes(dense_parts, sems.at[12])
    await_bytes(dense_down_w, sems.at[4])
    whole = jnp.sum(dense_parts[...].astype(jnp.float32), axis=0)
    dense_hidden = (whole[0] / (1.0 + jnp.exp(-whole[0])) * whole[1]).astype(jnp.bfloat16)

    def send_other(k, carry):
        send_out(lax.rem(tp + k, tp_count), 0)
        return carry

    lax.fori_loop(1, tp_count, send_other, 0)

    def own_tile(t, carry):
        cols = pl.ds(pl.multiple_of(t * step, LANES), step)
        dense = jnp.dot(dense_hidden, dense_down_w[:, cols], preferred_element_type=jnp.float32)
        put(tp, t, expert_cols(tp, t) + branch_factor * dense)
        return carry

    lax.fori_loop(0, col_width // step, own_tile, 0)
    to_sibling(tp)
    send_out(tp, 1)
    arrived[chip] = chip_out[tp, own_row]
    await_bytes(arrived.at[pl.ds(0, chips - 1)], sems.at[15])

    def gather_sum(i, total):
        return total + jnp.sum(arrived[pl.ds(i * 8, 8)].astype(jnp.float32), axis=0)

    out_ref[...] = lax.fori_loop(0, chips // 8, gather_sum, mixed_ref[...]).astype(out_ref.dtype)
    await_bytes(partials.at[pl.ds(0, tp_count - 1)], sems.at[5])
    if experts > 1:
        await_bytes(gathered.at[0, pl.ds(0, experts - 1), 0], sems.at[7])
    await_bytes(gathered.at[0, :, pl.ds(0, places - 1)], sems.at[8])
    await_bytes(gathered.at[0], sems.at[9])
    await_bytes(dense_parts.at[pl.ds(0, tp_count - 1)], sems.at[11])
    await_bytes(sibling_in, sems.at[13])
    await_bytes(arrived.at[pl.ds(0, chips - 1)], sems.at[14])


def tail(*operands):
    *arrays, ep_count, tp_count = operands
    heads, tokens = arrays[0], arrays[1]
    out_weight = arrays[5]
    expert_gate, expert_down, dense_gate, dense_down = arrays[6], arrays[8], arrays[9], arrays[11]
    rows, width = tokens.shape
    token_count = ep_count * rows
    col_width = width // tp_count
    expert_hidden = expert_gate.shape[2]
    dense_hidden = dense_gate.shape[0]
    experts = ep_count // QUARTERS
    head_width = heads.shape[1]
    head_chunks = head_width // min(CHUNK, head_width)
    bf16, f32 = jnp.bfloat16, jnp.float32
    vmem = pl.BlockSpec(memory_space=pltpu.VMEM)
    in_hbm = pl.BlockSpec(memory_space=pltpu.HBM)
    return pl.pallas_call(
        functools.partial(tail_kernel, ep_count, tp_count),
        out_shape=jax.ShapeDtypeStruct((rows, col_width), bf16),
        in_specs=[vmem] * 5 + [in_hbm] * 7,
        out_specs=vmem,
        scratch_shapes=[
            pltpu.VMEM((tp_count, head_width, col_width), bf16),
            pltpu.VMEM((expert_hidden // LANES, width, 2 * LANES), bf16),
            pltpu.VMEM(expert_down.shape[1:], bf16),
            pltpu.VMEM(dense_gate.shape, bf16),
            pltpu.VMEM(dense_gate.shape, bf16),
            pltpu.VMEM(dense_down.shape, bf16),
            pltpu.VMEM((tp_count - 1, rows, col_width), f32),
            pltpu.VMEM((tp_count, rows, col_width), f32),
            pltpu.VMEM((rows, col_width), f32),
            pltpu.VMEM((2, experts, 2 * tp_count, rows, col_width + LANES), bf16),
            pltpu.VMEM((token_count, width), bf16),
            pltpu.VMEM((2, token_count, dense_hidden), bf16),
            pltpu.VMEM((tp_count, 2, token_count, dense_hidden), bf16),
            pltpu.VMEM((token_count, expert_hidden), bf16),
            pltpu.VMEM((tp_count, 2, 2 * experts, rows, col_width), bf16),
            pltpu.VMEM((tp_count, 2 * experts, rows, col_width), bf16),
            pltpu.VMEM((tp_count, 2 * experts, rows, col_width), bf16),
            pltpu.VMEM((experts * 2 * tp_count, rows, col_width), bf16),
            pltpu.SemaphoreType.DMA((16,)),
            pltpu.SemaphoreType.DMA((tp_count * head_chunks,)),
            pltpu.SemaphoreType.DMA((experts,)),
            pltpu.SemaphoreType.DMA((experts,)),
            pltpu.SemaphoreType.DMA((tp_count,)),
        ],
        compiler_params=pltpu.CompilerParams(
            collective_id=0, has_side_effects=True, vmem_limit_bytes=62 * 1024 * 1024
        ),
    )(*arrays)


def local(
    tokens,
    past_lengths,
    state,
    norm1_gain,
    query_weight,
    key_weight,
    value_weight,
    out_weight,
    norm2_gain,
    branch_gate,
    route_ids,
    route_weights,
    expert_gate,
    expert_up,
    expert_down,
    dense_gate,
    dense_up,
    dense_down,
):
    tp_count = lax.axis_size("tp")
    ep_count = lax.axis_size("ep")
    heads_here = state.shape[1]
    head_index = lax.axis_index("tp") * heads_here + jnp.arange(heads_here)
    inputs = tokens.astype(jnp.float32)
    normed_in = (
        inputs
        * lax.rsqrt(jnp.mean(inputs * inputs, axis=-1, keepdims=True) + RMS_EPSILON)
        * norm1_gain
    ).astype(jnp.bfloat16)
    normed, new_state = retention_step(
        normed_in,
        past_lengths,
        state,
        query_weight,
        key_weight,
        value_weight,
        head_index,
        heads_here * tp_count,
    )
    lanes = jnp.arange(LANES, dtype=jnp.int32)
    named = (route_ids[:, :, None] == lanes[None, None, :]).astype(jnp.float32)
    route_lanes = jnp.sum(named * route_weights[:, :, None], axis=1)
    hidden_pad = -expert_gate.shape[2] % LANES
    if hidden_pad:
        expert_gate = jnp.pad(expert_gate, ((0, 0), (0, 0), (0, hidden_pad)))
        expert_up = jnp.pad(expert_up, ((0, 0), (0, 0), (0, hidden_pad)))
        expert_down = jnp.pad(expert_down, ((0, 0), (0, hidden_pad), (0, 0)))
    layer_out = tail(
        normed,
        tokens,
        norm2_gain[None, :],
        branch_gate[None, :],
        route_lanes,
        out_weight,
        expert_gate,
        expert_up,
        expert_down,
        dense_gate.T,
        dense_up.T,
        dense_down,
        ep_count,
        tp_count,
    )
    return (layer_out, new_state)


def solution(mesh):
    return jax.shard_map(
        local,
        mesh=mesh,
        in_specs=(
            P("ep", None),
            P("ep"),
            P("ep", "tp", None, None),
            P(),
            P(None, "tp"),
            P(None, "tp"),
            P(None, "tp"),
            P("tp", None),
            P(),
            P(),
            P("ep", None),
            P("ep", None),
            P("ep", None, "tp"),
            P("ep", None, "tp"),
            P("ep", "tp", None),
            P("tp", "ep"),
            P("tp", "ep"),
            P("ep", "tp"),
        ),
        out_specs=(P("ep", "tp"), P("ep", "tp", None, None)),
        check_vma=False,
    )
```
